32 devices in a mesh: sp: 8 (over z, x), tp: 4 (over y, core).
Axes of the slice: x: 2, y: 2, z: 4, core: 2. Of those that a mesh axis runs over, the one named last changes fastest.
Arguments:
- queries: bfloat16 [2048, 1536], P('sp', 'tp'), may hold values from -500 to 500
- latent: bfloat16 [2048, 256], P('sp'), may hold values from -6 to 6
- rope_key: bfloat16 [2048, 32], P('sp'), may hold values from -6 to 6
- latent_gain: bfloat16 [256], replicated, may hold values from 0.099609375 to 1.8984375
- key_value_weight: bfloat16 [256, 2048], P(None, 'tp'), may hold values from -0.375 to 0.375
- out_weight: bfloat16 [1024, 2048], P(None, 'tp'), may hold values from -6 to 6
- residual: bfloat16 [2048, 2048], P('sp', 'tp'), may hold values from -150 to 150
- ffn_gain: bfloat16 [2048], replicated, may hold values from 0.099609375 to 1.8984375
- routes: int32 [2048, 2], P('sp'), may hold values from 0 to 7, all different within a row; in each aligned block of 256 rows (0 to 255, 256 to 511, ...) at most 128 rows name the same one
- route_prob: float32 [2048, 2], P('sp'), may hold values from 0.1 to 1
- group_weight: float32 [2048], P('sp'), may hold values from 0.25 to 1
- gate_weight: bfloat16 [8, 2048, 4096], P('sp', None, 'tp'), may hold values from -0.125 to 0.125
- up_weight: bfloat16 [8, 2048, 4096], P('sp', None, 'tp'), may hold values from -0.125 to 0.125
- down_weight: bfloat16 [8, 4096, 2048], P('sp', None, 'tp'), may hold values from -0.75 to 0.75
Outputs:
- final: bfloat16 [2048, 2048], P('sp', 'tp')
The draws below stay inside these ranges and needn't reach their ends.
Inputs may be any that keep to these rules, and one draw needn't show every extreme that they name: `routes`: each row names 2 different experts; among the 256 rows of one index of sp no expert is named more than 128 times, a bound that some block reaches.
All inputs are finite; a program needn't handle non-finite values.
Results may differ from the reference program's by a relative error of at most 0.015.
The reference program's roundings to bfloat16 on the way count: a program that leaves them out, or rounds other values in their place, can miss the bound.
Values may be sent and summed in bfloat16 or wider, within the bound.
A program may use at most 64 MiB of HBM per device.

```python
import math
import jax
import jax.numpy as jnp
import numpy as np
from jax import lax

D = 2048
HEADS = 16
NOPE = 64
ROPE = 32
VDIM = 64
RANK = 256
FF = 4096
TOP = 2
SPAN = 64
TOK_SP = 256
TOKENS = 2048
EXPERTS = 8
CAP = 128
N_SP = 8


def draw_residual(key, part):
    keys = jax.random.split(jax.random.fold_in(key, 11), 3)
    base = jnp.clip(jax.random.normal(keys[0], (TOKENS, D), jnp.float32), -6.0, 6.0)
    column = jnp.exp(math.log(4.0) * jnp.arange(D, dtype=jnp.float32) / D)
    column = column * jax.random.uniform(keys[1], (D,), jnp.float32, 0.7, 1.3)
    rows = jnp.exp(jax.random.uniform(keys[2], (TOKENS, 1), jnp.float32, math.log(0.5), math.log(2.0)))
    return (base * rows * column[None, :]).astype(jnp.bfloat16)


def draw_queries(key, part):
    keys = jax.random.split(jax.random.fold_in(key, 23), 1)
    base = jnp.clip(jax.random.normal(keys[0], (TOKENS, HEADS * (NOPE + ROPE)), jnp.float32), -6.0, 6.0)
    return base.astype(jnp.bfloat16)


def block_scale(own_key, extent, pieces, least, largest):
    def one(axis_at, shards_of):
        heights = jax.random.uniform(jax.random.fold_in(jax.random.fold_in(own_key, 6), axis_at), (shards_of,), jnp.float32, least / len(pieces), largest / len(pieces))
        return jnp.repeat(jnp.exp(heights), extent[axis_at] // shards_of).reshape((-1,) + (1,) * (len(extent) - axis_at - 1))

    level = one(*pieces[0])
    for cut in pieces[1:]:
        level = level * one(*cut)
    return level


def shared_out(own_key, own, number, rows, count, top, bound, lean):
    order = jax.random.permutation(own_key, count)
    crowded, usual = portions_of(count, rows * top, bound, lean, True), portions_of(count, rows * top, bound, lean, False)
    places = jnp.arange(count)

    def named(lengths, offset_by):
        used = int((lengths > 0).sum())
        fixed = max(1, used // 4)
        moved = fixed + (places - fixed + offset_by * (used - fixed)) % max(1, count - fixed)
        return jnp.zeros((count,), jnp.int32).at[order[jnp.where(places < fixed, places, moved)]].set(jnp.asarray(lengths, jnp.int32))

    lengths = jnp.where(number % 4 == 0, named(crowded, number // 4), named(usual, number - number // 4 - 1))
    mixed = jax.random.permutation(jax.random.fold_in(own, 3), count)
    donor, receiver = mixed[0:count // 2 * 2:2], mixed[1:count // 2 * 2:2]
    slack = jnp.minimum(lengths[donor] - 1, bound - lengths[receiver]) // 2
    slack = jnp.where((donor == order[0]) | (receiver == order[0]) | (lengths[receiver] == 0), 0, jnp.maximum(slack, 0))
    moved = jax.random.randint(jax.random.fold_in(own, 4), (count // 2,), 0, 1 << 20) % (slack + 1)
    lengths = lengths.at[donor].add(-moved).at[receiver].add(moved)
    members = jnp.searchsorted(jnp.cumsum(lengths), jnp.arange(rows * top), side="right").astype(jnp.int32)
    table = members.reshape(top, rows).T
    table = table[jax.random.permutation(jax.random.fold_in(own, 1), rows)]
    offset_by = jax.random.randint(jax.random.fold_in(own, 2), (rows, 1), 0, top)
    return jnp.take_along_axis(table, (jnp.arange(top)[None, :] + offset_by) % top, axis=1)


def portions_of(amount, total, reach, slope, full):
    portions = [(1 << 20) // math.isqrt(grade ** slope) + 1 for grade in range(1, amount + 1)]
    largest = reach if full else min(reach, max(-(-total // amount), total * portions[0] // sum(portions)))
    least = 1 if total - largest >= amount - 1 else 0
    counts, spare = [largest] + [least] * (amount - 1), total - largest - least * (amount - 1)
    while spare > 0:
        movable = [i for i in range(1, amount) if counts[i] < largest] or [i for i in range(1, amount) if counts[i] < reach]
        mass, budget = sum([portions[i] for i in movable]), spare
        for i in movable:
            more = min(reach - counts[i], max(1, budget * portions[i] // mass), spare)
            counts[i] = counts[i] + more
            spare = spare - more
    return np.array(counts)


def normal_values(own_key, extent, spread, bound, cuts=(), kind=jnp.bfloat16):
    array = jax.random.normal(own_key, extent, jnp.float32) * spread
    if len(cuts) > 0:
        array = block_scale(own_key, extent, cuts, -0.22, 0.18) * array
    return jnp.clip(array, min=-bound, max=bound).astype(kind)


def setup_inputs(seed: int = 0) -> dict:
    splits = jax.random.split(jax.random.key(seed), 15)
    queries = draw_queries(jax.random.fold_in(splits[14], 71), 0)
    latent = normal_values(splits[1], (TOKENS, RANK), 1.0, 6.0, ((0, 8),))
    rope_key = normal_values(splits[2], (TOKENS, ROPE), 1.0, 6.0, ((0, 8),))
    latent_gain = jnp.clip(1.0 + 0.18 * jax.random.normal(splits[3], (RANK,), jnp.float32), 0.099609375, 1.8984375).astype(jnp.bfloat16)
    key_value_weight = normal_values(splits[4], (RANK, HEADS * (NOPE + VDIM)), RANK ** -0.5, 0.375, ((1, 4),))
    out_weight = normal_values(splits[5], (HEADS * VDIM, D), 1.0, 6.0, ((1, 4),))
    residual = draw_residual(jax.random.fold_in(splits[14], 71), 0)
    ffn_gain = jnp.clip(1.0 + 0.18 * jax.random.normal(splits[7], (D,), jnp.float32), 0.099609375, 1.8984375).astype(jnp.bfloat16)
    routes_keys = jax.random.split(jax.random.fold_in(splits[8], 1), TOKENS // TOK_SP)
    routes_turns = jax.random.permutation(jax.random.fold_in(splits[8], 3), TOKENS // TOK_SP)
    routes = jax.vmap(lambda own, number: shared_out(jax.random.fold_in(splits[8], 2), own, number, TOK_SP, EXPERTS, TOP, CAP, 1))(routes_keys, routes_turns).reshape((TOKENS, TOP))
    route_prob = jnp.clip(jnp.exp(math.log(1.0) - 2.3025851 * jax.random.uniform(splits[9], (TOKENS, TOP), jnp.float32) ** block_scale(splits[9], (TOKENS, TOP), ((0, 8),), -0.2, 0.2)), 0.1, 1.0)
    group_weight = jnp.clip(0.25 + 0.75 * jax.random.uniform(splits[10], (TOKENS,), jnp.float32) ** block_scale(splits[10], (TOKENS,), ((0, 8),), -0.2, 0.2), 0.25, 1.0)
    gate_weight = normal_values(splits[11], (EXPERTS, D, FF), D ** -0.5, 0.125, ((0, 8), (2, 4)))
    up_weight = normal_values(splits[12], (EXPERTS, D, FF), D ** -0.5, 0.125, ((0, 8), (2, 4)))
    down_weight = normal_values(splits[13], (EXPERTS, FF, D), (FF // 64) ** -0.5, 0.75, ((0, 8), (2, 4)))
    return {"queries": queries, "latent": latent, "rope_key": rope_key, "latent_gain": latent_gain, "key_value_weight": key_value_weight, "out_weight": out_weight, "residual": residual, "ffn_gain": ffn_gain, "routes": routes, "route_prob": route_prob, "group_weight": group_weight, "gate_weight": gate_weight, "up_weight": up_weight, "down_weight": down_weight}


THETA = 500000.0
EPSILON = 1e-06

def rotate(values, positions):
    rot_width = values.shape[-1]
    half_width = rot_width // 2
    frequency = 1.0 / THETA ** (jnp.arange(0, rot_width, 2, dtype=jnp.float32) / rot_width)
    angles = positions.astype(jnp.float32)[:, None] * frequency[None, :]
    view_shape = (values.shape[0],) + (1,) * (values.ndim - 2) + (half_width,)
    cos_table = jnp.cos(angles).reshape(view_shape)
    sin_table = jnp.sin(angles).reshape(view_shape)
    wide = values.astype(jnp.float32)
    lower_half = wide[..., :half_width]
    upper_half = wide[..., half_width:]
    return jnp.concatenate([lower_half * cos_table - upper_half * sin_table, upper_half * cos_table + lower_half * sin_table], axis=-1)

def reference(queries, latent, rope_key, latent_gain, key_value_weight, out_weight, residual, ffn_gain, routes, route_prob, group_weight, gate_weight, up_weight, down_weight):
    count = queries.shape[0]
    positions = jnp.arange(count, dtype=jnp.int32)
    query = queries.reshape(count, HEADS, NOPE + ROPE)
    query = jnp.concatenate([query[..., :NOPE].astype(jnp.float32), rotate(query[..., NOPE:], positions)], axis=-1).astype(jnp.bfloat16)
    latent_wide = latent.astype(jnp.float32)
    normed = latent_wide * lax.rsqrt(lax.optimization_barrier(jnp.mean(latent_wide * latent_wide, axis=-1, keepdims=True)) + EPSILON)
    normed = (normed * latent_gain.astype(jnp.float32)).astype(jnp.bfloat16)
    key_value = jnp.dot(normed, key_value_weight, preferred_element_type=jnp.float32).astype(jnp.bfloat16).reshape(count, HEADS, NOPE + VDIM)
    rotated = rotate(rope_key, positions).astype(jnp.bfloat16)
    key_nope = key_value[..., :NOPE].astype(jnp.float32)
    values = key_value[..., NOPE:].astype(jnp.float32)
    rotated_wide = rotated.astype(jnp.float32)
    key_blocks = positions // SPAN
    query_block = math.gcd(count, 512)
    scaling = (NOPE + ROPE) ** (-0.5)

    def one_block(block_index):
        first_row = (block_index * query_block).astype(jnp.int32)
        part = lax.dynamic_slice_in_dim(query, first_row, query_block, 0).astype(jnp.float32)
        scores = jnp.einsum('qhd,khd->hqk', part[..., :NOPE], key_nope)
        scores = scores + jnp.einsum('qhd,kd->hqk', part[..., NOPE:], rotated_wide)
        scores = scores * scaling
        query_blocks = (first_row + jnp.arange(query_block, dtype=jnp.int32)) // SPAN
        allowed = key_blocks[None, :] <= query_blocks[:, None]
        scores = jnp.where(allowed[None, :, :], scores, -jnp.inf)
        row_max = lax.optimization_barrier(jnp.max(scores, axis=-1, keepdims=True))
        expd = jnp.exp(scores - row_max)
        denom = lax.optimization_barrier(jnp.sum(expd, axis=-1))
        weights_half = expd.astype(jnp.bfloat16).astype(jnp.float32)
        summed = jnp.einsum('hqk,khd->qhd', weights_half, values)
        return (summed / jnp.transpose(denom)[..., None]).astype(jnp.bfloat16)
    attended = lax.map(one_block, jnp.arange(count // query_block, dtype=jnp.int32)).reshape(count, HEADS * VDIM)
    mixed = (residual.astype(jnp.float32) + jnp.dot(attended, out_weight, preferred_element_type=jnp.float32)).astype(jnp.bfloat16)
    mixed_wide = mixed.astype(jnp.float32)
    row_scale = lax.rsqrt(lax.optimization_barrier(jnp.mean(mixed_wide * mixed_wide, axis=-1)) + EPSILON)
    scaled = (mixed_wide * ffn_gain.astype(jnp.float32)).astype(jnp.bfloat16)
    picks = routes.reshape(N_SP, TOK_SP * TOP)
    onehot = (picks[:, :, None] == jnp.arange(EXPERTS, dtype=jnp.int32)[None, None, :]).astype(jnp.int32)
    slot_index = lax.optimization_barrier(jnp.sum((jnp.cumsum(onehot, axis=1) - 1) * onehot, axis=2))
    group_index = jnp.arange(N_SP, dtype=jnp.int32)[:, None]
    target = (picks * (N_SP * CAP) + group_index * CAP + slot_index).reshape(-1).astype(jnp.int32)
    token_of = jnp.arange(count * TOP, dtype=jnp.int32) // TOP
    buffer = jnp.zeros((EXPERTS * N_SP * CAP, D), jnp.bfloat16).at[target].set(scaled[token_of])
    scale_buffer = jnp.zeros((EXPERTS * N_SP * CAP,), jnp.float32).at[target].set(row_scale[token_of])

    def run_expert(operands):
        rows, scales, gate_one, up_one, down_one = operands
        gate_acc = scales[:, None] * jnp.dot(rows, gate_one, preferred_element_type=jnp.float32)
        up_acc = scales[:, None] * jnp.dot(rows, up_one, preferred_element_type=jnp.float32)
        hidden = (jax.nn.silu(gate_acc) * up_acc).astype(jnp.bfloat16)
        return jnp.dot(hidden, down_one, preferred_element_type=jnp.float32).astype(jnp.bfloat16)
    expert_out = lax.map(run_expert, (buffer.reshape(EXPERTS, N_SP * CAP, D), scale_buffer.reshape(EXPERTS, N_SP * CAP), gate_weight, up_weight, down_weight))
    picked = expert_out.reshape(EXPERTS * N_SP * CAP, D)[target].astype(jnp.float32).reshape(count, TOP, D)
    combine = group_weight[:, None] * route_prob / lax.optimization_barrier(jnp.sum(route_prob, axis=-1, keepdims=True))
    routed_sum = lax.optimization_barrier(jnp.sum(combine[..., None] * picked, axis=1))
    return (mixed_wide + routed_sum).astype(jnp.bfloat16)
```

```python
import functools
import jax
import jax.numpy as jnp
from jax import lax
from jax.experimental import pallas as pl
from jax.experimental.pallas import tpu as pltpu
from jax.sharding import PartitionSpec as P

NOPE = 64
ROPE = 32
VDIM = 64
TOP = 2
SPAN = 64
GROUPS = 4
LANES = 128


THETA = 500000.0
EPSILON = 1e-06
MESH = pl.DeviceIdType.MESH


def rotate(values, positions):
    rot_width = values.shape[-1]
    half_width = rot_width // 2
    frequency = 1.0 / THETA ** (jnp.arange(0, rot_width, 2, dtype=jnp.float32) / rot_width)
    angles = positions.astype(jnp.float32)[:, None] * frequency[None, :]
    view_shape = (values.shape[0],) + (1,) * (values.ndim - 2) + (half_width,)
    cos_table = jnp.cos(angles).reshape(view_shape)
    sin_table = jnp.sin(angles).reshape(view_shape)
    wide = values.astype(jnp.float32)
    lower_half = wide[..., :half_width]
    upper_half = wide[..., half_width:]
    return jnp.concatenate(
        [
            lower_half * cos_table - upper_half * sin_table,
            upper_half * cos_table + lower_half * sin_table,
        ],
        axis=-1,
    )


class Links:
    def __init__(self, n_sp, n_tp, send_sem, recv_sem):
        self.n_sp, self.ny = n_sp, n_tp // 2
        self.sp, self.tp = lax.axis_index("sp"), lax.axis_index("tp")
        self.y, self.core = self.tp // 2, self.tp % 2
        self.send_sem, self.recv_sem = send_sem, recv_sem
        self.copies = []

    def barrier(self, over_sp):
        barrier = pltpu.get_barrier_semaphore()
        peers = [(self.sp, self.row(j)) for j in range(1, self.ny)] + [(self.sp, self.twin())]
        if over_sp:
            peers += [((self.sp + r) % self.n_sp, self.tp) for r in range(1, self.n_sp)]
        for peer in peers:
            pl.semaphore_signal(barrier, inc=1, device_id=peer, device_id_type=MESH)
        pl.semaphore_wait(barrier, len(peers))

    def row(self, j):
        return ((self.y + j) % self.ny) * 2 + self.core

    def twin(self):
        return self.y * 2 + (1 - self.core)

    def send(self, src, dst, sp, tp):
        k = len(self.copies)
        copy = pltpu.make_async_remote_copy(
            src_ref=src,
            dst_ref=dst,
            send_sem=self.send_sem.at[k],
            recv_sem=self.recv_sem.at[k],
            device_id=(sp, tp),
            device_id_type=MESH,
        )
        copy.start()
        self.copies.append(copy)
        return copy

    def close(self):
        for copy in self.copies:
            copy.wait_send()


class Spread:
    def __init__(self, links, bufs, g):
        self.links, self.bufs, self.g = links, bufs, g

    def start(self):
        ln = self.links
        self.rows, self.twins = [], []
        for buf in self.bufs:
            mine = buf.at[self.g, ln.tp]
            self.rows.append([ln.send(mine, mine, ln.sp, ln.row(j)) for j in range(1, ln.ny)])
            self.twins.append(ln.send(mine, mine, ln.sp, ln.twin()))

    def relay(self):
        ln = self.links
        for buf, rows in zip(self.bufs, self.rows):
            for j, copy in enumerate(rows, 1):
                copy.wait_recv()
                piece = buf.at[self.g, ln.row(ln.ny - j)]
                self.twins.append(ln.send(piece, piece, ln.sp, ln.twin()))

    def finish(self):
        for copy in self.twins:
            copy.wait_recv()


def copies_of(n_sp, n_tp, groups, exchanged, spreads):
    return exchanged * (n_sp - 1) + spreads * groups * (n_tp - 1)


def latent_kernel(n_sp, n_tp, block_ref, buf, send_sem, recv_sem, local_sem):
    rows = block_ref.shape[0]
    per = n_sp // GROUPS
    links = Links(n_sp, n_tp, send_sem, recv_sem)
    links.barrier(True)
    own = pltpu.make_async_copy(block_ref, buf.at[0, links.tp, pl.ds(0, rows)], local_sem)
    own.start()
    arriving = [own]
    for r in range(1, n_sp):
        g, i = divmod(r, per)
        dst = buf.at[g, links.tp, pl.ds(i * rows, rows)]
        arriving.append(links.send(block_ref, dst, (links.sp + n_sp - r) % n_sp, links.tp))
    spreads = [Spread(links, (buf,), g) for g in range(GROUPS)]
    for g in range(GROUPS):
        for i in range(per):
            r = g * per + i
            if r == 0:
                own.wait()
            else:
                arriving[r].wait_recv()
        spreads[g].start()
        if g > 0:
            spreads[g - 1].relay()
    spreads[-1].relay()
    for spread in spreads:
        spread.finish()
    links.close()


def gather_latents(block, n_sp, n_tp):
    rows, width = block.shape
    count = copies_of(n_sp, n_tp, GROUPS, 1, 1)
    return pl.pallas_call(
        functools.partial(latent_kernel, n_sp, n_tp),
        out_shape=jax.ShapeDtypeStruct((GROUPS, n_tp, n_sp // GROUPS * rows, width), block.dtype),
        in_specs=[pl.BlockSpec(memory_space=pltpu.VMEM)],
        out_specs=pl.BlockSpec(memory_space=pltpu.VMEM),
        scratch_shapes=[
            pltpu.SemaphoreType.DMA((count,)),
            pltpu.SemaphoreType.DMA((count,)),
            pltpu.SemaphoreType.DMA,
        ],
        compiler_params=pltpu.CompilerParams(collective_id=0, has_side_effects=True),
        name="gather_latents",
    )(block)


def attended_kernel(n_sp, n_tp, att_ref, weight_ref, resid_ref, mixed_ref, buf, send_sem, recv_sem, local_sem):
    links = Links(n_sp, n_tp, send_sem, recv_sem)
    depth = att_ref.shape[1]
    links.barrier(False)
    own = pltpu.make_async_copy(att_ref, buf.at[0, links.tp], local_sem)
    own.start()
    own.wait()
    spread = Spread(links, (buf,), 0)
    spread.start()
    spread.relay()
    spread.finish()
    total = jnp.zeros(mixed_ref.shape, jnp.float32)
    for t in range(n_tp):
        total = total + jnp.dot(
            buf[0, t], weight_ref[t * depth : (t + 1) * depth, :], preferred_element_type=jnp.float32
        )
    mixed_ref[...] = (resid_ref[...].astype(jnp.float32) + total).astype(jnp.bfloat16)
    links.close()


def project_attended(attended, weight, residual, n_sp, n_tp):
    count = copies_of(n_sp, n_tp, 1, 0, 1)
    return pl.pallas_call(
        functools.partial(attended_kernel, n_sp, n_tp),
        out_shape=jax.ShapeDtypeStruct(residual.shape, residual.dtype),
        in_specs=[pl.BlockSpec(memory_space=pltpu.VMEM)] * 3,
        out_specs=pl.BlockSpec(memory_space=pltpu.VMEM),
        scratch_shapes=[
            pltpu.VMEM((1, n_tp) + attended.shape, attended.dtype),
            pltpu.SemaphoreType.DMA((count,)),
            pltpu.SemaphoreType.DMA((count,)),
            pltpu.SemaphoreType.DMA,
        ],
        compiler_params=pltpu.CompilerParams(collective_id=1, has_side_effects=True),
        name="project_attended",
    )(attended, weight, residual)


def expert_kernel(
    n_sp, n_tp, placed_ref, squares_ref, gate_hbm, up_hbm, down_hbm, ret_ref,
    rx, sq, hid, ostage, gate_w, up_w, down_w, send_sem, recv_sem, local_sem,
):
    cap, width = placed_ref.shape[1:]
    per = n_sp // GROUPS
    d_model = width * n_tp
    hidden_here = gate_w.shape[1]
    links = Links(n_sp, n_tp, send_sem, recv_sem)
    links.barrier(True)
    own = pltpu.make_async_copy(placed_ref.at[0], rx.at[0, links.tp, pl.ds(0, cap)], local_sem.at[0])
    own_sq = pltpu.make_async_copy(squares_ref.at[0], sq.at[0, links.tp, 0], local_sem.at[1])
    own.start()
    own_sq.start()
    arriving = [None]
    for r in range(1, n_sp):
        g, i = divmod(r, per)
        target = (links.sp + n_sp - r) % n_sp
        arriving.append((
            links.send(squares_ref.at[r], sq.at[g, links.tp, i], target, links.tp),
            links.send(placed_ref.at[r], rx.at[g, links.tp, pl.ds(i * cap, cap)], target, links.tp),
        ))
    loads = [
        pltpu.make_async_copy(gate_hbm.at[0], gate_w, local_sem.at[2]),
        pltpu.make_async_copy(up_hbm.at[0], up_w, local_sem.at[3]),
        pltpu.make_async_copy(down_hbm.at[0], down_w, local_sem.at[4]),
    ]
    for load in loads:
        load.start()
    inputs = [Spread(links, (sq, rx), g) for g in range(GROUPS)]
    hiddens = [Spread(links, (hid,), g) for g in range(GROUPS)]
    returning = []

    def arrive(g):
        for i in range(per):
            r = g * per + i
            if r == 0:
                own.wait()
                own_sq.wait()
            else:
                for copy in arriving[r]:
                    copy.wait_recv()
        inputs[g].start()

    def up_stage(g):
        inputs[g].relay()
        inputs[g].finish()
        if g == 0:
            loads[0].wait()
            loads[1].wait()
        columns = []
        for i in range(per):
            lanes = sq[g, 0, i]
            for t in range(1, n_tp):
                lanes = lanes + sq[g, t, i]
            scale = lax.rsqrt(lanes / d_model + EPSILON)
            columns.append(jnp.broadcast_to(scale[0:1, :], (LANES, LANES)).T[:cap, 0:1])
        scale = jnp.concatenate(columns, axis=0)
        tile = min(256, hidden_here)

        @pl.loop(0, hidden_here // tile)
        def _(n):
            cols = pl.ds(pl.multiple_of(n * tile, tile), tile)
            gate = jnp.zeros((per * cap, tile), jnp.float32)
            upper = jnp.zeros((per * cap, tile), jnp.float32)
            for t in range(n_tp):
                rows = rx[g, t]
                depth = pl.ds(t * width, width)
                gate = gate + jnp.dot(rows, gate_w[depth, cols], preferred_element_type=jnp.float32)
                upper = upper + jnp.dot(rows, up_w[depth, cols], preferred_element_type=jnp.float32)
            gate = gate * scale
            upper = upper * scale
            value = gate / (1.0 + jnp.exp(-gate)) * upper
            hid[g, links.tp, :, cols] = value.astype(jnp.bfloat16)

        hiddens[g].start()

    def down_stage(g):
        hiddens[g].relay()
        hiddens[g].finish()
        if g == 0:
            loads[2].wait()
        tile = min(256, width)

        @pl.loop(0, width // tile)
        def _(n):
            cols = pl.ds(pl.multiple_of(n * tile, tile), tile)
            total = jnp.zeros((per * cap, tile), jnp.float32)
            for t in range(n_tp):
                total = total + jnp.dot(
                    hid[g, t],
                    down_w[pl.ds(t * hidden_here, hidden_here), cols],
                    preferred_element_type=jnp.float32,
                )
            ostage[g, :, cols] = total.astype(jnp.bfloat16)

        for i in range(per):
            r = g * per + i
            piece = ostage.at[g, pl.ds(i * cap, cap)]
            if r == 0:
                back = pltpu.make_async_copy(piece, ret_ref.at[0], local_sem.at[5])
                back.start()
                returning.append(back)
            else:
                returning.append(
                    links.send(piece, ret_ref.at[r], (links.sp + r) % n_sp, links.tp)
                )

    arrive(0)
    arrive(1)
    up_stage(0)
    for g in range(2, GROUPS):
        arrive(g)
        up_stage(g - 1)
    down_stage(0)
    up_stage(GROUPS - 1)
    for g in range(1, GROUPS):
        down_stage(g)
    returning[0].wait()
    for copy in returning[1:]:
        copy.wait_recv()
    links.close()


def run_experts(placed, squares, gate_weight, up_weight, down_weight, n_sp, n_tp):
    cap, width = placed.shape[1:]
    per = n_sp // GROUPS
    hidden_here = gate_weight.shape[2]
    count = copies_of(n_sp, n_tp, GROUPS, 3, 3)
    vmem = pl.BlockSpec(memory_space=pltpu.VMEM)
    hbm = pl.BlockSpec(memory_space=pl.ANY)
    return pl.pallas_call(
        functools.partial(expert_kernel, n_sp, n_tp),
        out_shape=jax.ShapeDtypeStruct(placed.shape, placed.dtype),
        in_specs=[vmem, vmem, hbm, hbm, hbm],
        out_specs=vmem,
        scratch_shapes=[
            pltpu.VMEM((GROUPS, n_tp, per * cap, width), jnp.bfloat16),
            pltpu.VMEM((GROUPS, n_tp, per) + squares.shape[1:], jnp.float32),
            pltpu.VMEM((GROUPS, n_tp, per * cap, hidden_here), jnp.bfloat16),
            pltpu.VMEM((GROUPS, per * cap, width), jnp.bfloat16),
            pltpu.VMEM(gate_weight.shape[1:], jnp.bfloat16),
            pltpu.VMEM(up_weight.shape[1:], jnp.bfloat16),
            pltpu.VMEM(down_weight.shape[1:], jnp.bfloat16),
            pltpu.SemaphoreType.DMA((count,)),
            pltpu.SemaphoreType.DMA((count,)),
            pltpu.SemaphoreType.DMA((6,)),
        ],
        compiler_params=pltpu.CompilerParams(
            collective_id=2, has_side_effects=True, vmem_limit_bytes=50 * 1024 * 1024
        ),
        name="run_experts",
    )(placed, squares, gate_weight, up_weight, down_weight)


def body(
    queries,
    latent,
    rope_key,
    latent_gain,
    key_value_weight,
    out_weight,
    residual,
    ffn_gain,
    routes,
    route_prob,
    group_weight,
    gate_weight,
    up_weight,
    down_weight,
):
    n_sp, n_tp = lax.axis_size("sp"), lax.axis_size("tp")
    sp, tp = lax.axis_index("sp"), lax.axis_index("tp")
    tokens_here, rank = latent.shape
    heads_here = key_value_weight.shape[1] // (NOPE + VDIM)
    width_here = residual.shape[1]
    length = n_sp * tokens_here
    quarter = tokens_here // n_tp

    pad = -(rank + ROPE) % LANES
    block = jnp.concatenate(
        [latent, rope_key, jnp.zeros((tokens_here, pad), latent.dtype)], axis=1
    )
    block = lax.dynamic_slice_in_dim(block, tp * quarter, quarter, 0)
    per = n_sp // GROUPS
    gathered = gather_latents(block, n_sp, n_tp)
    gathered = gathered.reshape(length, rank + ROPE + pad)
    index = jnp.arange(length, dtype=jnp.int32)
    in_quarter = index % quarter
    in_group = index // quarter % per
    of_tp = index // (quarter * per) % n_tp
    group = index // (quarter * per * n_tp)
    source = (sp + group * per + in_group) % n_sp
    key_positions = source * tokens_here + of_tp * quarter + in_quarter

    positions = sp * tokens_here + jnp.arange(tokens_here, dtype=jnp.int32)
    query = queries.reshape(tokens_here, heads_here, NOPE + ROPE)
    query_nope = query[..., :NOPE]
    query_rope = rotate(query[..., NOPE:], positions).astype(jnp.bfloat16)
    scaling = (NOPE + ROPE) ** (-0.5)
    latent_wide = gathered[:, :rank].astype(jnp.float32)
    normed = latent_wide * lax.rsqrt(
        jnp.mean(latent_wide * latent_wide, axis=-1, keepdims=True) + EPSILON
    )
    normed = (normed * latent_gain.astype(jnp.float32)).astype(jnp.bfloat16)
    key_value = jnp.dot(normed, key_value_weight, preferred_element_type=jnp.float32).astype(
        jnp.bfloat16
    )
    rotated = rotate(gathered[:, rank : rank + ROPE], key_positions).astype(jnp.bfloat16)
    key_value = key_value.reshape(length, heads_here, NOPE + VDIM)
    scores = jnp.einsum(
        "qhd,khd->qhk", query_nope, key_value[..., :NOPE], preferred_element_type=jnp.float32
    )
    scores = scores + jnp.einsum(
        "qhd,kd->qhk", query_rope, rotated, preferred_element_type=jnp.float32
    )
    scores = scores * scaling
    allowed = (key_positions // SPAN)[None, :] <= (positions // SPAN)[:, None]
    scores = jnp.where(allowed[:, None, :], scores, -jnp.inf)
    row_max = jnp.max(scores, axis=-1)
    exp_scores = jnp.exp(scores - row_max[..., None])
    normalizer = jnp.sum(exp_scores, axis=-1)
    weighted = jnp.einsum(
        "qhk,khd->qhd",
        exp_scores.astype(jnp.bfloat16),
        key_value[..., NOPE:],
        preferred_element_type=jnp.float32,
    )
    attended = (
        (weighted / normalizer[..., None])
        .astype(jnp.bfloat16)
        .reshape(tokens_here, heads_here * VDIM)
    )
    mixed_rows = project_attended(attended, out_weight, residual, n_sp, n_tp)
    mixed_wide = mixed_rows.astype(jnp.float32)

    capacity = 2 * tokens_here * TOP // n_sp
    picks = routes.reshape(-1)
    onehot = (picks[:, None] == jnp.arange(n_sp, dtype=jnp.int32)[None, :]).astype(jnp.int32)
    slot_index = jnp.sum((jnp.cumsum(onehot, axis=0) - 1) * onehot, axis=1)
    target = ((sp + n_sp - picks) % n_sp * capacity + slot_index).reshape(tokens_here, TOP)
    slots = jnp.arange(n_sp * capacity, dtype=jnp.int32)
    chosen = [target[:, k][None, :] == slots[:, None] for k in range(TOP)]
    anywhere = functools.reduce(jnp.logical_or, chosen)

    part_squares = jnp.sum(mixed_wide * mixed_wide, axis=-1)
    slot_squares = jnp.sum(jnp.where(anywhere, part_squares[None, :], 0.0), axis=1)
    slot_squares = jnp.pad(
        slot_squares.reshape(n_sp, 1, capacity), ((0, 0), (0, 0), (0, LANES - capacity))
    )
    slot_squares = jnp.broadcast_to(slot_squares, (n_sp, 8, LANES))
    gain_here = lax.dynamic_slice_in_dim(ffn_gain, tp * width_here, width_here, 0).astype(
        jnp.float32
    )
    scaled = (mixed_wide * gain_here[None, :]).astype(jnp.bfloat16)
    placed = jnp.dot(
        anywhere.astype(jnp.bfloat16), scaled, preferred_element_type=jnp.float32
    ).astype(jnp.bfloat16)
    returned = run_experts(
        placed.reshape(n_sp, capacity, width_here),
        slot_squares,
        gate_weight,
        up_weight,
        down_weight,
        n_sp,
        n_tp,
    ).reshape(n_sp * capacity, width_here)
    combine = group_weight[:, None] * route_prob / jnp.sum(route_prob, axis=-1, keepdims=True)
    total = mixed_wide
    routed_sum = jnp.zeros_like(mixed_wide)
    for k in range(TOP):
        picked = lax.dot_general(
            chosen[k].astype(jnp.bfloat16),
            returned,
            (((0,), (0,)), ((), ())),
            preferred_element_type=jnp.float32,
        )
        routed_sum = routed_sum + combine[:, k : k + 1] * picked
    return (total + routed_sum).astype(jnp.bfloat16)


def solution(mesh):
    return jax.shard_map(
        body,
        mesh=mesh,
        in_specs=(
            P("sp", "tp"),
            P("sp", None),
            P("sp", None),
            P(),
            P(None, "tp"),
            P(None, "tp"),
            P("sp", "tp"),
            P(),
            P("sp", None),
            P("sp", None),
            P("sp"),
            P("sp", None, "tp"),
            P("sp", None, "tp"),
            P("sp", None, "tp"),
        ),
        out_specs=P("sp", "tp"),
        check_vma=False,
    )
```

```python
import functools
import jax
import jax.numpy as jnp
from jax import lax
from jax.experimental import pallas as pl
from jax.experimental.pallas import tpu as pltpu
from jax.sharding import PartitionSpec as P

NOPE = 64
ROPE = 32
VDIM = 64
TOP = 2
SPAN = 64
GROUPS = 4
LANES = 128


THETA = 500000.0
EPSILON = 1e-06
MESH = pl.DeviceIdType.MESH


def rotate(values, positions):
    rot_width = values.shape[-1]
    half_width = rot_width // 2
    frequency = 1.0 / THETA ** (jnp.arange(0, rot_width, 2, dtype=jnp.float32) / rot_width)
    angles = positions.astype(jnp.float32)[:, None] * frequency[None, :]
    view_shape = (values.shape[0],) + (1,) * (values.ndim - 2) + (half_width,)
    cos_table = jnp.cos(angles).reshape(view_shape)
    sin_table = jnp.sin(angles).reshape(view_shape)
    wide = values.astype(jnp.float32)
    lower_half = wide[..., :half_width]
    upper_half = wide[..., half_width:]
    return jnp.concatenate(
        [
            lower_half * cos_table - upper_half * sin_table,
            upper_half * cos_table + lower_half * sin_table,
        ],
        axis=-1,
    )


class Links:
    def __init__(self, n_sp, n_tp, send_sem, recv_sem):
        self.n_sp, self.ny = n_sp, n_tp // 2
        self.sp, self.tp = lax.axis_index("sp"), lax.axis_index("tp")
        self.y, self.core = self.tp // 2, self.tp % 2
        self.send_sem, self.recv_sem = send_sem, recv_sem
        self.copies = []

    def barrier(self, over_sp):
        barrier = pltpu.get_barrier_semaphore()
        peers = [(self.sp, self.row(j)) for j in range(1, self.ny)] + [(self.sp, self.twin())]
        if over_sp:
            peers += [((self.sp + r) % self.n_sp, self.tp) for r in range(1, self.n_sp)]
        for peer in peers:
            pl.semaphore_signal(barrier, inc=1, device_id=peer, device_id_type=MESH)
        pl.semaphore_wait(barrier, len(peers))

    def row(self, j):
        return ((self.y + j) % self.ny) * 2 + self.core

    def twin(self):
        return self.y * 2 + (1 - self.core)

    def send(self, src, dst, sp, tp):
        k = len(self.copies)
        copy = pltpu.make_async_remote_copy(
            src_ref=src,
            dst_ref=dst,
            send_sem=self.send_sem.at[k],
            recv_sem=self.recv_sem.at[k],
            device_id=(sp, tp),
            device_id_type=MESH,
        )
        copy.start()
        self.copies.append(copy)
        return copy

    def close(self):
        for copy in self.copies:
            copy.wait_send()


class Spread:
    def __init__(self, links, bufs, g, source=None):
        self.links, self.bufs, self.g, self.source = links, bufs, g, source

    def start(self):
        ln = self.links
        self.rows, self.twins = [], []
        for buf in self.bufs:
            mine = buf.at[self.g, ln.tp]
            src = mine if self.source is None else self.source
            self.rows.append([ln.send(src, mine, ln.sp, ln.row(j)) for j in range(1, ln.ny)])
            self.twins.append(ln.send(src, mine, ln.sp, ln.twin()))

    def relay(self):
        ln = self.links
        for buf, rows in zip(self.bufs, self.rows):
            for j, copy in enumerate(rows, 1):
                copy.wait_recv()
                piece = buf.at[self.g, ln.row(ln.ny - j)]
                self.twins.append(ln.send(piece, piece, ln.sp, ln.twin()))

    def finish(self):
        for copy in self.twins:
            copy.wait_recv()


def copies_of(n_sp, n_tp, groups, exchanged, spreads):
    return exchanged * (n_sp - 1) + spreads * groups * (n_tp - 1)


def latent_kernel(n_sp, n_tp, block_ref, buf, send_sem, recv_sem, local_sem):
    rows = block_ref.shape[0]
    per = n_sp // GROUPS
    links = Links(n_sp, n_tp, send_sem, recv_sem)
    links.barrier(True)
    own = pltpu.make_async_copy(block_ref, buf.at[0, links.tp, pl.ds(0, rows)], local_sem)
    own.start()
    arriving = [own]
    for r in range(1, n_sp):
        g, i = divmod(r, per)
        dst = buf.at[g, links.tp, pl.ds(i * rows, rows)]
        arriving.append(links.send(block_ref, dst, (links.sp + n_sp - r) % n_sp, links.tp))
    spreads = [Spread(links, (buf,), g) for g in range(GROUPS)]
    for g in range(GROUPS):
        for i in range(per):
            r = g * per + i
            if r == 0:
                own.wait()
            else:
                arriving[r].wait_recv()
        spreads[g].start()
        if g > 0:
            spreads[g - 1].relay()
    spreads[-1].relay()
    for spread in spreads:
        spread.finish()
    links.close()


def gather_latents(block, n_sp, n_tp):
    rows, width = block.shape
    count = copies_of(n_sp, n_tp, GROUPS, 1, 1)
    return pl.pallas_call(
        functools.partial(latent_kernel, n_sp, n_tp),
        out_shape=jax.ShapeDtypeStruct((GROUPS, n_tp, n_sp // GROUPS * rows, width), block.dtype),
        in_specs=[pl.BlockSpec(memory_space=pltpu.VMEM)],
        out_specs=pl.BlockSpec(memory_space=pltpu.VMEM),
        scratch_shapes=[
            pltpu.SemaphoreType.DMA((count,)),
            pltpu.SemaphoreType.DMA((count,)),
            pltpu.SemaphoreType.DMA,
        ],
        compiler_params=pltpu.CompilerParams(collective_id=0, has_side_effects=True),
        name="gather_latents",
    )(block)


def attended_kernel(n_sp, n_tp, att_ref, weight_ref, resid_ref, mixed_ref, mine, buf, send_sem, recv_sem, local_sem):
    links = Links(n_sp, n_tp, send_sem, recv_sem)
    depth = att_ref.shape[1]
    links.barrier(False)
    own = pltpu.make_async_copy(att_ref, mine, local_sem)
    own.start()
    own.wait()
    half = att_ref.shape[0] // 2
    spreads = [Spread(links, (buf,), g, mine.at[pl.ds(g * half, half)]) for g in range(2)]
    for spread in spreads:
        spread.start()
    for spread in spreads:
        spread.relay()
    for g, spread in enumerate(spreads):
        spread.finish()
        buf[g, links.tp] = mine[g * half : (g + 1) * half, :]
        total = resid_ref[g * half : (g + 1) * half, :].astype(jnp.float32)
        summed = jnp.zeros(total.shape, jnp.float32)
        for t in range(n_tp):
            summed = summed + jnp.dot(
                buf[g, t],
                weight_ref[t * depth : (t + 1) * depth, :],
                preferred_element_type=jnp.float32,
            )
        mixed_ref[g * half : (g + 1) * half, :] = (total + summed).astype(jnp.bfloat16)
    links.close()


def project_attended(attended, weight, residual, n_sp, n_tp):
    count = copies_of(n_sp, n_tp, 2, 0, 1)
    return pl.pallas_call(
        functools.partial(attended_kernel, n_sp, n_tp),
        out_shape=jax.ShapeDtypeStruct(residual.shape, residual.dtype),
        in_specs=[pl.BlockSpec(memory_space=pltpu.VMEM)] * 3,
        out_specs=pl.BlockSpec(memory_space=pltpu.VMEM),
        scratch_shapes=[
            pltpu.VMEM(attended.shape, attended.dtype),
            pltpu.VMEM((2, n_tp, attended.shape[0] // 2, attended.shape[1]), attended.dtype),
            pltpu.SemaphoreType.DMA((count,)),
            pltpu.SemaphoreType.DMA((count,)),
            pltpu.SemaphoreType.DMA,
        ],
        compiler_params=pltpu.CompilerParams(collective_id=1, has_side_effects=True),
        name="project_attended",
    )(attended, weight, residual)


def expert_kernel(
    n_sp, n_tp, placed_ref, squares_ref, gate_hbm, up_hbm, down_hbm, across_hbm, ret_ref,
    rx, sq, hid, own_sum, part_out, part_in, ostage,
    gate_w, up_w, down_w, across_w, send_sem, recv_sem, local_sem,
):
    cap, width = placed_ref.shape[1:]
    per = n_sp // GROUPS
    d_model = width * n_tp
    hidden_here = gate_w.shape[1]
    deep = 2 * hidden_here
    links = Links(n_sp, n_tp, send_sem, recv_sem)
    links.barrier(True)
    own = pltpu.make_async_copy(placed_ref.at[0], rx.at[0, links.tp, pl.ds(0, cap)], local_sem.at[0])
    own_sq = pltpu.make_async_copy(squares_ref.at[0], sq.at[0, links.tp, 0], local_sem.at[1])
    own.start()
    own_sq.start()
    arriving = [None]
    for r in range(1, n_sp):
        g, i = divmod(r, per)
        target = (links.sp + n_sp - r) % n_sp
        arriving.append((
            links.send(squares_ref.at[r], sq.at[g, links.tp, i], target, links.tp),
            links.send(placed_ref.at[r], rx.at[g, links.tp, pl.ds(i * cap, cap)], target, links.tp),
        ))
    loads = [
        pltpu.make_async_copy(gate_hbm.at[0], gate_w, local_sem.at[2]),
        pltpu.make_async_copy(up_hbm.at[0], up_w, local_sem.at[3]),
        pltpu.make_async_copy(across_hbm, across_w, local_sem.at[4]),
        pltpu.make_async_copy(
            down_hbm.at[0, pl.ds(pl.multiple_of(links.y * deep, 128), deep)], down_w, local_sem.at[6]
        ),
    ]
    for load in loads:
        load.start()
    inputs = [Spread(links, (sq, rx), g) for g in range(GROUPS)]
    twins = {}
    parts = {}
    returning = []

    def arrive(g):
        for i in range(per):
            r = g * per + i
            if r == 0:
                own.wait()
                own_sq.wait()
            else:
                for copy in arriving[r]:
                    copy.wait_recv()
        inputs[g].start()

    def up_stage(g):
        inputs[g].relay()
        inputs[g].finish()
        if g == 0:
            loads[0].wait()
            loads[1].wait()
        columns = []
        for i in range(per):
            lanes = sq[g, 0, i]
            for t in range(1, n_tp):
                lanes = lanes + sq[g, t, i]
            scale = lax.rsqrt(lanes / d_model + EPSILON)
            columns.append(jnp.broadcast_to(scale[0:1, :], (LANES, LANES)).T[:cap, 0:1])
        scale = jnp.concatenate(columns, axis=0)
        tile = min(256, hidden_here)

        @pl.loop(0, hidden_here // tile)
        def _(n):
            cols = pl.ds(pl.multiple_of(n * tile, tile), tile)
            gate = jnp.zeros((per * cap, tile), jnp.float32)
            upper = jnp.zeros((per * cap, tile), jnp.float32)
            for t in range(n_tp):
                rows = rx[g, t]
                depth = pl.ds(t * width, width)
                gate = gate + jnp.dot(rows, gate_w[depth, cols], preferred_element_type=jnp.float32)
                upper = upper + jnp.dot(rows, up_w[depth, cols], preferred_element_type=jnp.float32)
            gate = gate * scale
            upper = upper * scale
            value = gate / (1.0 + jnp.exp(-gate)) * upper
            hid[g, links.core, :, cols] = value.astype(jnp.bfloat16)

        half = hid.at[g, links.core]
        twins[g] = links.send(half, half, links.sp, links.twin())

    tile_out = min(256, width)

    def product(g, weight, cols):
        total = jnp.zeros((per * cap, tile_out), jnp.float32)
        for c in range(2):
            total = total + jnp.dot(
                hid[g, c],
                weight[pl.ds(c * hidden_here, hidden_here), cols],
                preferred_element_type=jnp.float32,
            )
        return total

    def down_stage(g):
        twins[g].wait_recv()
        if g == 0:
            loads[2].wait()
        parts[g] = []
        for j in range(1, links.ny):

            @pl.loop(0, width // tile_out)
            def _(n):
                cols = pl.ds(pl.multiple_of(n * tile_out, tile_out), tile_out)
                part_out[g, j - 1, :, cols] = product(g, across_w.at[j - 1], cols).astype(
                    jnp.bfloat16
                )

            parts[g].append(
                links.send(part_out.at[g, j - 1], part_in.at[g, j - 1], links.sp, links.row(j))
            )
        if g == 0:
            loads[3].wait()

        @pl.loop(0, width // tile_out)
        def _(n):
            cols = pl.ds(pl.multiple_of(n * tile_out, tile_out), tile_out)
            own_sum[g, :, cols] = product(g, down_w, cols)

    def return_stage(g):
        total = own_sum[g]
        for j, copy in enumerate(parts[g]):
            copy.wait_recv()
            total = total + part_in[g, j].astype(jnp.float32)
        ostage[g] = total.astype(jnp.bfloat16)
        for i in range(per):
            r = g * per + i
            piece = ostage.at[g, pl.ds(i * cap, cap)]
            if r == 0:
                back = pltpu.make_async_copy(piece, ret_ref.at[0], local_sem.at[5])
                back.start()
                returning.append(back)
            else:
                returning.append(
                    links.send(piece, ret_ref.at[r], (links.sp + r) % n_sp, links.tp)
                )

    arrive(0)
    arrive(1)
    up_stage(0)
    for g in range(2, GROUPS):
        arrive(g)
        up_stage(g - 1)
        down_stage(g - 2)
    up_stage(GROUPS - 1)
    down_stage(GROUPS - 2)
    return_stage(0)
    down_stage(GROUPS - 1)
    for g in range(1, GROUPS):
        return_stage(g)
    returning[0].wait()
    for copy in returning[1:]:
        copy.wait_recv()
    links.close()


def run_experts(placed, squares, gate_weight, up_weight, down_weight, across, n_sp, n_tp):
    cap, width = placed.shape[1:]
    per = n_sp // GROUPS
    hidden_here = gate_weight.shape[2]
    ny = n_tp // 2
    count = copies_of(n_sp, n_tp, GROUPS, 3, 2) + GROUPS * ny
    vmem = pl.BlockSpec(memory_space=pltpu.VMEM)
    hbm = pl.BlockSpec(memory_space=pl.ANY)
    return pl.pallas_call(
        functools.partial(expert_kernel, n_sp, n_tp),
        out_shape=jax.ShapeDtypeStruct(placed.shape, placed.dtype),
        in_specs=[vmem, vmem, hbm, hbm, hbm, hbm],
        out_specs=vmem,
        scratch_shapes=[
            pltpu.VMEM((GROUPS, n_tp, per * cap, width), jnp.bfloat16),
            pltpu.VMEM((GROUPS, n_tp, per) + squares.shape[1:], jnp.float32),
            pltpu.VMEM((GROUPS, 2, per * cap, hidden_here), jnp.bfloat16),
            pltpu.VMEM((GROUPS, per * cap, width), jnp.float32),
            pltpu.VMEM((GROUPS, ny - 1, per * cap, width), jnp.bfloat16),
            pltpu.VMEM((GROUPS, ny - 1, per * cap, width), jnp.bfloat16),
            pltpu.VMEM((GROUPS, per * cap, width), jnp.bfloat16),
            pltpu.VMEM(gate_weight.shape[1:], jnp.bfloat16),
            pltpu.VMEM(up_weight.shape[1:], jnp.bfloat16),
            pltpu.VMEM((2 * hidden_here, width), jnp.bfloat16),
            pltpu.VMEM(across.shape, jnp.bfloat16),
            pltpu.SemaphoreType.DMA((count,)),
            pltpu.SemaphoreType.DMA((count,)),
            pltpu.SemaphoreType.DMA((7,)),
        ],
        compiler_params=pltpu.CompilerParams(
            collective_id=2, has_side_effects=True, vmem_limit_bytes=50 * 1024 * 1024
        ),
        name="run_experts",
    )(placed, squares, gate_weight, up_weight, down_weight, across)


def body(
    queries,
    latent,
    rope_key,
    latent_gain,
    key_value_weight,
    out_weight,
    residual,
    ffn_gain,
    routes,
    route_prob,
    group_weight,
    gate_weight,
    up_weight,
    down_weight,
):
    n_sp, n_tp = lax.axis_size("sp"), lax.axis_size("tp")
    sp, tp = lax.axis_index("sp"), lax.axis_index("tp")
    tokens_here, rank = latent.shape
    heads_here = key_value_weight.shape[1] // (NOPE + VDIM)
    width_here = residual.shape[1]
    length = n_sp * tokens_here
    quarter = tokens_here // n_tp

    ny, deep = n_tp // 2, 2 * gate_weight.shape[2]
    across = []
    for j in range(1, ny):
        there = (tp // 2 + j) % ny
        rows = lax.dynamic_slice_in_dim(down_weight[0], there * deep, deep, 0)
        pairs = [(t, (t // 2 + j) % ny * 2 + t % 2) for t in range(n_tp)]
        across.append(lax.ppermute(rows, "tp", pairs))
    across = across[::-1]

    rope_rows = -(-quarter * ROPE // rank)
    pad = -rope_rows % 8
    rope_part = lax.dynamic_slice_in_dim(rope_key, tp * quarter, quarter, 0)
    block = jnp.concatenate(
        [
            lax.dynamic_slice_in_dim(latent, tp * quarter, quarter, 0),
            rope_part.reshape(rope_rows, rank),
            jnp.zeros((pad, rank), latent.dtype),
        ],
        axis=0,
    )
    per = n_sp // GROUPS
    gathered = gather_latents(block, n_sp, n_tp)
    gathered = gathered.reshape(n_sp * n_tp, quarter + rope_rows + pad, rank)
    latent_all = gathered[:, :quarter].reshape(length, rank)
    rope_all = gathered[:, quarter : quarter + rope_rows].reshape(length, ROPE)
    index = jnp.arange(length, dtype=jnp.int32)
    in_quarter = index % quarter
    in_group = index // quarter % per
    of_tp = index // (quarter * per) % n_tp
    group = index // (quarter * per * n_tp)
    source = (sp + group * per + in_group) % n_sp
    key_positions = source * tokens_here + of_tp * quarter + in_quarter

    positions = sp * tokens_here + jnp.arange(tokens_here, dtype=jnp.int32)
    query = queries.reshape(tokens_here, heads_here, NOPE + ROPE)
    query_nope = query[..., :NOPE]
    query_rope = rotate(query[..., NOPE:], positions).astype(jnp.bfloat16)
    scaling = (NOPE + ROPE) ** (-0.5)
    latent_wide = latent_all.astype(jnp.float32)
    normed = latent_wide * lax.rsqrt(
        jnp.mean(latent_wide * latent_wide, axis=-1, keepdims=True) + EPSILON
    )
    normed = (normed * latent_gain.astype(jnp.float32)).astype(jnp.bfloat16)
    key_value = jnp.dot(normed, key_value_weight, preferred_element_type=jnp.float32).astype(
        jnp.bfloat16
    )
    rotated = rotate(rope_all, key_positions).astype(jnp.bfloat16)
    key_value = key_value.reshape(length, heads_here, NOPE + VDIM)
    scores = jnp.einsum(
        "qhd,khd->qhk", query_nope, key_value[..., :NOPE], preferred_element_type=jnp.float32
    )
    scores = scores + jnp.einsum(
        "qhd,kd->qhk", query_rope, rotated, preferred_element_type=jnp.float32
    )
    scores = scores * scaling
    allowed = (key_positions // SPAN)[None, :] <= (positions // SPAN)[:, None]
    scores = jnp.where(allowed[:, None, :], scores, -jnp.inf)
    row_max = jnp.max(scores, axis=-1)
    exp_scores = jnp.exp(scores - row_max[..., None])
    normalizer = jnp.sum(exp_scores, axis=-1)
    weighted = jnp.einsum(
        "qhk,khd->qhd",
        exp_scores.astype(jnp.bfloat16),
        key_value[..., NOPE:],
        preferred_element_type=jnp.float32,
    )
    attended = (
        (weighted / normalizer[..., None])
        .astype(jnp.bfloat16)
        .reshape(tokens_here, heads_here * VDIM)
    )
    mixed_rows = project_attended(attended, out_weight, residual, n_sp, n_tp)
    mixed_wide = mixed_rows.astype(jnp.float32)

    capacity = 2 * tokens_here * TOP // n_sp
    picks = routes.reshape(-1)
    onehot = (picks[:, None] == jnp.arange(n_sp, dtype=jnp.int32)[None, :]).astype(jnp.int32)
    slot_index = jnp.sum((jnp.cumsum(onehot, axis=0) - 1) * onehot, axis=1)
    target = ((sp + n_sp - picks) % n_sp * capacity + slot_index).reshape(tokens_here, TOP)
    slots = jnp.arange(n_sp * capacity, dtype=jnp.int32)
    chosen = [target[:, k][None, :] == slots[:, None] for k in range(TOP)]
    anywhere = functools.reduce(jnp.logical_or, chosen)

    part_squares = jnp.sum(mixed_wide * mixed_wide, axis=-1)
    slot_squares = jnp.sum(jnp.where(anywhere, part_squares[None, :], 0.0), axis=1)
    slot_squares = jnp.pad(
        slot_squares.reshape(n_sp, 1, capacity), ((0, 0), (0, 0), (0, LANES - capacity))
    )
    slot_squares = jnp.broadcast_to(slot_squares, (n_sp, 8, LANES))
    gain_here = lax.dynamic_slice_in_dim(ffn_gain, tp * width_here, width_here, 0).astype(
        jnp.float32
    )
    scaled = (mixed_wide * gain_here[None, :]).astype(jnp.bfloat16)
    placed = jnp.dot(
        anywhere.astype(jnp.bfloat16), scaled, preferred_element_type=jnp.float32
    ).astype(jnp.bfloat16)
    returned = run_experts(
        placed.reshape(n_sp, capacity, width_here),
        slot_squares,
        gate_weight,
        up_weight,
        down_weight,
        jnp.stack(across),
        n_sp,
        n_tp,
    ).reshape(n_sp * capacity, width_here)
    combine = group_weight[:, None] * route_prob / jnp.sum(route_prob, axis=-1, keepdims=True)
    total = mixed_wide
    routed_sum = jnp.zeros_like(mixed_wide)
    for k in range(TOP):
        picked = lax.dot_general(
            chosen[k].astype(jnp.bfloat16),
            returned,
            (((0,), (0,)), ((), ())),
            preferred_element_type=jnp.float32,
        )
        routed_sum = routed_sum + combine[:, k : k + 1] * picked
    return (total + routed_sum).astype(jnp.bfloat16)


def solution(mesh):
    return jax.shard_map(
        body,
        mesh=mesh,
        in_specs=(
            P("sp", "tp"),
            P("sp", None),
            P("sp", None),
            P(),
            P(None, "tp"),
            P(None, "tp"),
            P("sp", "tp"),
            P(),
            P("sp", None),
            P("sp", None),
            P("sp"),
            P("sp", None, "tp"),
            P("sp", None, "tp"),
            P("sp", None, "tp"),
        ),
        out_specs=P("sp", "tp"),
        check_vma=False,
    )
```

```python
import functools
import jax
import jax.numpy as jnp
from jax import lax
from jax.experimental import pallas as pl
from jax.experimental.pallas import tpu as pltpu
from jax.sharding import PartitionSpec as P

NOPE = 64
ROPE = 32
VDIM = 64
TOP = 2
SPAN = 64
GROUPS = 4
LANES = 128


THETA = 500000.0
EPSILON = 1e-06
MESH = pl.DeviceIdType.MESH


def rotate(values, positions):
    rot_width = values.shape[-1]
    half_width = rot_width // 2
    frequency = 1.0 / THETA ** (jnp.arange(0, rot_width, 2, dtype=jnp.float32) / rot_width)
    angles = positions.astype(jnp.float32)[:, None] * frequency[None, :]
    view_shape = (values.shape[0],) + (1,) * (values.ndim - 2) + (half_width,)
    cos_table = jnp.cos(angles).reshape(view_shape)
    sin_table = jnp.sin(angles).reshape(view_shape)
    wide = values.astype(jnp.float32)
    lower_half = wide[..., :half_width]
    upper_half = wide[..., half_width:]
    return jnp.concatenate(
        [
            lower_half * cos_table - upper_half * sin_table,
            upper_half * cos_table + lower_half * sin_table,
        ],
        axis=-1,
    )


class Links:
    def __init__(self, n_sp, n_tp, send_sem, recv_sem):
        self.n_sp, self.ny = n_sp, n_tp // 2
        self.sp, self.tp = lax.axis_index("sp"), lax.axis_index("tp")
        self.y, self.core = self.tp // 2, self.tp % 2
        self.send_sem, self.recv_sem = send_sem, recv_sem
        self.copies = []

    def barrier(self, over_sp):
        barrier = pltpu.get_barrier_semaphore()
        peers = [(self.sp, self.row(j)) for j in range(1, self.ny)] + [(self.sp, self.twin())]
        if over_sp:
            peers += [((self.sp + r) % self.n_sp, self.tp) for r in range(1, self.n_sp)]
        for peer in peers:
            pl.semaphore_signal(barrier, inc=1, device_id=peer, device_id_type=MESH)
        pl.semaphore_wait(barrier, len(peers))

    def row(self, j):
        return ((self.y + j) % self.ny) * 2 + self.core

    def twin(self):
        return self.y * 2 + (1 - self.core)

    def send(self, src, dst, sp, tp):
        k = len(self.copies)
        copy = pltpu.make_async_remote_copy(
            src_ref=src,
            dst_ref=dst,
            send_sem=self.send_sem.at[k],
            recv_sem=self.recv_sem.at[k],
            device_id=(sp, tp),
            device_id_type=MESH,
        )
        copy.start()
        self.copies.append(copy)
        return copy

    def close(self):
        for copy in self.copies:
            copy.wait_send()


class Spread:
    def __init__(self, links, bufs, g, source=None):
        self.links, self.bufs, self.g, self.source = links, bufs, g, source

    def start(self):
        ln = self.links
        self.rows, self.twins = [], []
        for buf in self.bufs:
            mine = buf.at[self.g, ln.tp]
            src = mine if self.source is None else self.source
            self.rows.append([ln.send(src, mine, ln.sp, ln.row(j)) for j in range(1, ln.ny)])
            self.twins.append(ln.send(src, mine, ln.sp, ln.twin()))

    def relay(self):
        ln = self.links
        for buf, rows in zip(self.bufs, self.rows):
            for j, copy in enumerate(rows, 1):
                copy.wait_recv()
                piece = buf.at[self.g, ln.row(ln.ny - j)]
                self.twins.append(ln.send(piece, piece, ln.sp, ln.twin()))

    def finish(self):
        for copy in self.twins:
            copy.wait_recv()


def copies_of(n_sp, n_tp, groups, exchanged, spreads):
    return exchanged * (n_sp - 1) + spreads * groups * (n_tp - 1)


def latent_kernel(n_sp, n_tp, block_ref, buf, send_sem, recv_sem, local_sem):
    rows = block_ref.shape[0]
    per = n_sp // GROUPS
    links = Links(n_sp, n_tp, send_sem, recv_sem)
    links.barrier(True)
    own = pltpu.make_async_copy(block_ref, buf.at[0, links.core, pl.ds(0, rows)], local_sem)
    own.start()
    arriving = [own]
    for r in range(1, n_sp):
        g, i = divmod(r, per)
        dst = buf.at[g, links.core, pl.ds(i * rows, rows)]
        arriving.append(links.send(block_ref, dst, (links.sp + n_sp - r) % n_sp, links.tp))
    twins = []
    for g in range(GROUPS):
        for i in range(per):
            r = g * per + i
            if r == 0:
                own.wait()
            else:
                arriving[r].wait_recv()
        half = buf.at[g, links.core]
        twins.append(links.send(half, half, links.sp, links.twin()))
    for copy in twins:
        copy.wait_recv()
    links.close()


def gather_latents(block, n_sp, n_tp):
    rows, width = block.shape
    count = n_sp - 1 + GROUPS
    return pl.pallas_call(
        functools.partial(latent_kernel, n_sp, n_tp),
        out_shape=jax.ShapeDtypeStruct((GROUPS, 2, n_sp // GROUPS * rows, width), block.dtype),
        in_specs=[pl.BlockSpec(memory_space=pltpu.VMEM)],
        out_specs=pl.BlockSpec(memory_space=pltpu.VMEM),
        scratch_shapes=[
            pltpu.SemaphoreType.DMA((count,)),
            pltpu.SemaphoreType.DMA((count,)),
            pltpu.SemaphoreType.DMA,
        ],
        compiler_params=pltpu.CompilerParams(collective_id=0, has_side_effects=True),
        name="gather_latents",
    )(block)


def attended_kernel(n_sp, n_tp, att_ref, weight_ref, resid_ref, mixed_ref, mine, buf, send_sem, recv_sem, local_sem):
    links = Links(n_sp, n_tp, send_sem, recv_sem)
    depth = att_ref.shape[1]
    links.barrier(False)
    own = pltpu.make_async_copy(att_ref, mine, local_sem)
    own.start()
    own.wait()
    half = att_ref.shape[0] // 2
    spreads = [Spread(links, (buf,), g, mine.at[pl.ds(g * half, half)]) for g in range(2)]
    for spread in spreads:
        spread.start()
    for spread in spreads:
        spread.relay()
    for g, spread in enumerate(spreads):
        spread.finish()
        buf[g, links.tp] = mine[g * half : (g + 1) * half, :]
        total = resid_ref[g * half : (g + 1) * half, :].astype(jnp.float32)
        summed = jnp.zeros(total.shape, jnp.float32)
        for t in range(n_tp):
            summed = summed + jnp.dot(
                buf[g, t],
                weight_ref[t * depth : (t + 1) * depth, :],
                preferred_element_type=jnp.float32,
            )
        mixed_ref[g * half : (g + 1) * half, :] = (total + summed).astype(jnp.bfloat16)
    links.close()


def project_attended(attended, weight, residual, n_sp, n_tp):
    count = copies_of(n_sp, n_tp, 2, 0, 1)
    return pl.pallas_call(
        functools.partial(attended_kernel, n_sp, n_tp),
        out_shape=jax.ShapeDtypeStruct(residual.shape, residual.dtype),
        in_specs=[pl.BlockSpec(memory_space=pltpu.VMEM)] * 3,
        out_specs=pl.BlockSpec(memory_space=pltpu.VMEM),
        scratch_shapes=[
            pltpu.VMEM(attended.shape, attended.dtype),
            pltpu.VMEM((2, n_tp, attended.shape[0] // 2, attended.shape[1]), attended.dtype),
            pltpu.SemaphoreType.DMA((count,)),
            pltpu.SemaphoreType.DMA((count,)),
            pltpu.SemaphoreType.DMA,
        ],
        compiler_params=pltpu.CompilerParams(collective_id=1, has_side_effects=True),
        name="project_attended",
    )(attended, weight, residual)


def expert_kernel(
    n_sp, n_tp, placed_ref, squares_ref, gate_hbm, up_hbm, down_hbm, across_hbm, ret_ref,
    rx, sq, hid, own_sum, part_out, part_in, ostage,
    gate_w, up_w, down_w, across_w, send_sem, recv_sem, local_sem,
):
    cap, width = placed_ref.shape[1:]
    per = n_sp // GROUPS
    d_model = width * n_tp
    hidden_here = gate_w.shape[1]
    deep = 2 * hidden_here
    links = Links(n_sp, n_tp, send_sem, recv_sem)
    links.barrier(True)
    own = pltpu.make_async_copy(placed_ref.at[0], rx.at[0, links.tp, pl.ds(0, cap)], local_sem.at[0])
    own_sq = pltpu.make_async_copy(squares_ref.at[0], sq.at[0, links.tp, 0], local_sem.at[1])
    own.start()
    own_sq.start()
    arriving = [None]
    for r in range(1, n_sp):
        g, i = divmod(r, per)
        target = (links.sp + n_sp - r) % n_sp
        arriving.append((
            links.send(squares_ref.at[r], sq.at[g, links.tp, i], target, links.tp),
            links.send(placed_ref.at[r], rx.at[g, links.tp, pl.ds(i * cap, cap)], target, links.tp),
        ))
    loads = [
        pltpu.make_async_copy(gate_hbm.at[0], gate_w, local_sem.at[2]),
        pltpu.make_async_copy(up_hbm.at[0], up_w, local_sem.at[3]),
        pltpu.make_async_copy(across_hbm, across_w, local_sem.at[4]),
        pltpu.make_async_copy(
            down_hbm.at[0, pl.ds(pl.multiple_of(links.y * deep, 128), deep)], down_w, local_sem.at[6]
        ),
    ]
    for load in loads:
        load.start()
    inputs = [Spread(links, (sq, rx), g) for g in range(GROUPS)]
    twins = {}
    parts = {}
    returning = []

    def arrive(g):
        for i in range(per):
            r = g * per + i
            if r == 0:
                own.wait()
                own_sq.wait()
            else:
                for copy in arriving[r]:
                    copy.wait_recv()
        inputs[g].start()

    def up_stage(g):
        inputs[g].relay()
        inputs[g].finish()
        if g == 0:
            loads[0].wait()
            loads[1].wait()
        columns = []
        for i in range(per):
            lanes = sq[g, 0, i]
            for t in range(1, n_tp):
                lanes = lanes + sq[g, t, i]
            scale = lax.rsqrt(lanes / d_model + EPSILON)
            columns.append(jnp.broadcast_to(scale[0:1, :], (LANES, LANES)).T[:cap, 0:1])
        scale = jnp.concatenate(columns, axis=0)
        tile = min(256, hidden_here)

        @pl.loop(0, hidden_here // tile)
        def _(n):
            cols = pl.ds(pl.multiple_of(n * tile, tile), tile)
            gate = jnp.zeros((per * cap, tile), jnp.float32)
            upper = jnp.zeros((per * cap, tile), jnp.float32)
            for t in range(n_tp):
                rows = rx[g, t]
                depth = pl.ds(t * width, width)
                gate = gate + jnp.dot(rows, gate_w[depth, cols], preferred_element_type=jnp.float32)
                upper = upper + jnp.dot(rows, up_w[depth, cols], preferred_element_type=jnp.float32)
            gate = gate * scale
            upper = upper * scale
            value = gate / (1.0 + jnp.exp(-gate)) * upper
            hid[g, links.core, :, cols] = value.astype(jnp.bfloat16)

        half = hid.at[g, links.core]
        twins[g] = links.send(half, half, links.sp, links.twin())

    tile_out = min(256, width)

    def product(g, weight, cols):
        total = jnp.zeros((per * cap, tile_out), jnp.float32)
        for c in range(2):
            total = total + jnp.dot(
                hid[g, c],
                weight[pl.ds(c * hidden_here, hidden_here), cols],
                preferred_element_type=jnp.float32,
            )
        return total

    def down_stage(g):
        twins[g].wait_recv()
        if g == 0:
            loads[2].wait()
        parts[g] = []
        for j in range(1, links.ny):

            @pl.loop(0, width // tile_out)
            def _(n):
                cols = pl.ds(pl.multiple_of(n * tile_out, tile_out), tile_out)
                part_out[g, j - 1, :, cols] = product(g, across_w.at[j - 1], cols).astype(
                    jnp.bfloat16
                )

            parts[g].append(
                links.send(part_out.at[g, j - 1], part_in.at[g, j - 1], links.sp, links.row(j))
            )
        if g == 0:
            loads[3].wait()

        @pl.loop(0, width // tile_out)
        def _(n):
            cols = pl.ds(pl.multiple_of(n * tile_out, tile_out), tile_out)
            own_sum[g, :, cols] = product(g, down_w, cols)

    def return_stage(g):
        total = own_sum[g]
        for j, copy in enumerate(parts[g]):
            copy.wait_recv()
            total = total + part_in[g, j].astype(jnp.float32)
        ostage[g] = total.astype(jnp.bfloat16)
        for i in range(per):
            r = g * per + i
            piece = ostage.at[g, pl.ds(i * cap, cap)]
            if r == 0:
                back = pltpu.make_async_copy(piece, ret_ref.at[0], local_sem.at[5])
                back.start()
                returning.append(back)
            else:
                returning.append(
                    links.send(piece, ret_ref.at[r], (links.sp + r) % n_sp, links.tp)
                )

    arrive(0)
    arrive(1)
    up_stage(0)
    for g in range(2, GROUPS):
        arrive(g)
        up_stage(g - 1)
        down_stage(g - 2)
    up_stage(GROUPS - 1)
    down_stage(GROUPS - 2)
    return_stage(0)
    down_stage(GROUPS - 1)
    for g in range(1, GROUPS):
        return_stage(g)
    returning[0].wait()
    for copy in returning[1:]:
        copy.wait_recv()
    links.close()


def run_experts(placed, squares, gate_weight, up_weight, down_weight, across, n_sp, n_tp):
    cap, width = placed.shape[1:]
    per = n_sp // GROUPS
    hidden_here = gate_weight.shape[2]
    ny = n_tp // 2
    count = copies_of(n_sp, n_tp, GROUPS, 3, 2) + GROUPS * ny
    vmem = pl.BlockSpec(memory_space=pltpu.VMEM)
    hbm = pl.BlockSpec(memory_space=pl.ANY)
    return pl.pallas_call(
        functools.partial(expert_kernel, n_sp, n_tp),
        out_shape=jax.ShapeDtypeStruct(placed.shape, placed.dtype),
        in_specs=[vmem, vmem, hbm, hbm, hbm, hbm],
        out_specs=vmem,
        scratch_shapes=[
            pltpu.VMEM((GROUPS, n_tp, per * cap, width), jnp.bfloat16),
            pltpu.VMEM((GROUPS, n_tp, per) + squares.shape[1:], jnp.float32),
            pltpu.VMEM((GROUPS, 2, per * cap, hidden_here), jnp.bfloat16),
            pltpu.VMEM((GROUPS, per * cap, width), jnp.float32),
            pltpu.VMEM((GROUPS, ny - 1, per * cap, width), jnp.bfloat16),
            pltpu.VMEM((GROUPS, ny - 1, per * cap, width), jnp.bfloat16),
            pltpu.VMEM((GROUPS, per * cap, width), jnp.bfloat16),
            pltpu.VMEM(gate_weight.shape[1:], jnp.bfloat16),
            pltpu.VMEM(up_weight.shape[1:], jnp.bfloat16),
            pltpu.VMEM((2 * hidden_here, width), jnp.bfloat16),
            pltpu.VMEM(across.shape, jnp.bfloat16),
            pltpu.SemaphoreType.DMA((count,)),
            pltpu.SemaphoreType.DMA((count,)),
            pltpu.SemaphoreType.DMA((7,)),
        ],
        compiler_params=pltpu.CompilerParams(
            collective_id=2, has_side_effects=True, vmem_limit_bytes=50 * 1024 * 1024
        ),
        name="run_experts",
    )(placed, squares, gate_weight, up_weight, down_weight, across)


def body(
    queries,
    latent,
    rope_key,
    latent_gain,
    key_value_weight,
    out_weight,
    residual,
    ffn_gain,
    routes,
    route_prob,
    group_weight,
    gate_weight,
    up_weight,
    down_weight,
):
    n_sp, n_tp = lax.axis_size("sp"), lax.axis_size("tp")
    sp, tp = lax.axis_index("sp"), lax.axis_index("tp")
    tokens_here, rank = latent.shape
    heads_here = key_value_weight.shape[1] // (NOPE + VDIM)
    width_here = residual.shape[1]
    length = n_sp * tokens_here
    part = tokens_here // 2

    ny, deep = n_tp // 2, 2 * gate_weight.shape[2]
    across = []
    for j in range(1, ny):
        there = (tp // 2 + j) % ny
        rows = lax.dynamic_slice_in_dim(down_weight[0], there * deep, deep, 0)
        pairs = [(t, (t // 2 + j) % ny * 2 + t % 2) for t in range(n_tp)]
        across.append(lax.ppermute(rows, "tp", pairs))
    across = across[::-1]

    pad = -(rank + ROPE) % LANES
    block = jnp.concatenate(
        [latent, rope_key, jnp.zeros((tokens_here, pad), latent.dtype)], axis=1
    )
    block = lax.dynamic_slice_in_dim(block, tp % 2 * part, part, 0)
    per = n_sp // GROUPS
    gathered = gather_latents(block, n_sp, n_tp)
    gathered = gathered.reshape(length, rank + ROPE + pad)
    index = jnp.arange(length, dtype=jnp.int32)
    in_part = index % part
    in_group = index // part % per
    of_core = index // (part * per) % 2
    group = index // (part * per * 2)
    source = (sp + group * per + in_group) % n_sp
    key_positions = source * tokens_here + of_core * part + in_part

    positions = sp * tokens_here + jnp.arange(tokens_here, dtype=jnp.int32)
    query = queries.reshape(tokens_here, heads_here, NOPE + ROPE)
    query_nope = query[..., :NOPE]
    query_rope = rotate(query[..., NOPE:], positions).astype(jnp.bfloat16)
    scaling = (NOPE + ROPE) ** (-0.5)
    latent_wide = gathered[:, :rank].astype(jnp.float32)
    normed = latent_wide * lax.rsqrt(
        jnp.mean(latent_wide * latent_wide, axis=-1, keepdims=True) + EPSILON
    )
    normed = (normed * latent_gain.astype(jnp.float32)).astype(jnp.bfloat16)
    key_value = jnp.dot(normed, key_value_weight, preferred_element_type=jnp.float32).astype(
        jnp.bfloat16
    )
    rotated = rotate(gathered[:, rank : rank + ROPE], key_positions).astype(jnp.bfloat16)
    key_value = key_value.reshape(length, heads_here, NOPE + VDIM)
    scores = jnp.einsum(
        "qhd,khd->qhk", query_nope, key_value[..., :NOPE], preferred_element_type=jnp.float32
    )
    scores = scores + jnp.einsum(
        "qhd,kd->qhk", query_rope, rotated, preferred_element_type=jnp.float32
    )
    scores = scores * scaling
    allowed = (key_positions // SPAN)[None, :] <= (positions // SPAN)[:, None]
    scores = jnp.where(allowed[:, None, :], scores, -jnp.inf)
    row_max = jnp.max(scores, axis=-1)
    exp_scores = jnp.exp(scores - row_max[..., None])
    normalizer = jnp.sum(exp_scores, axis=-1)
    weighted = jnp.einsum(
        "qhk,khd->qhd",
        exp_scores.astype(jnp.bfloat16),
        key_value[..., NOPE:],
        preferred_element_type=jnp.float32,
    )
    attended = (
        (weighted / normalizer[..., None])
        .astype(jnp.bfloat16)
        .reshape(tokens_here, heads_here * VDIM)
    )
    mixed_rows = project_attended(attended, out_weight, residual, n_sp, n_tp)
    mixed_wide = mixed_rows.astype(jnp.float32)

    capacity = 2 * tokens_here * TOP // n_sp
    picks = routes.reshape(-1)
    onehot = (picks[:, None] == jnp.arange(n_sp, dtype=jnp.int32)[None, :]).astype(jnp.int32)
    slot_index = jnp.sum((jnp.cumsum(onehot, axis=0) - 1) * onehot, axis=1)
    target = ((sp + n_sp - picks) % n_sp * capacity + slot_index).reshape(tokens_here, TOP)
    slots = jnp.arange(n_sp * capacity, dtype=jnp.int32)
    chosen = [target[:, k][None, :] == slots[:, None] for k in range(TOP)]
    anywhere = functools.reduce(jnp.logical_or, chosen)

    part_squares = jnp.sum(mixed_wide * mixed_wide, axis=-1)
    slot_squares = jnp.sum(jnp.where(anywhere, part_squares[None, :], 0.0), axis=1)
    slot_squares = jnp.pad(
        slot_squares.reshape(n_sp, 1, capacity), ((0, 0), (0, 0), (0, LANES - capacity))
    )
    slot_squares = jnp.broadcast_to(slot_squares, (n_sp, 8, LANES))
    gain_here = lax.dynamic_slice_in_dim(ffn_gain, tp * width_here, width_here, 0).astype(
        jnp.float32
    )
    scaled = (mixed_wide * gain_here[None, :]).astype(jnp.bfloat16)
    placed = jnp.dot(
        anywhere.astype(jnp.bfloat16), scaled, preferred_element_type=jnp.float32
    ).astype(jnp.bfloat16)
    returned = run_experts(
        placed.reshape(n_sp, capacity, width_here),
        slot_squares,
        gate_weight,
        up_weight,
        down_weight,
        jnp.stack(across),
        n_sp,
        n_tp,
    ).reshape(n_sp * capacity, width_here)
    combine = group_weight[:, None] * route_prob / jnp.sum(route_prob, axis=-1, keepdims=True)
    total = mixed_wide
    routed_sum = jnp.zeros_like(mixed_wide)
    for k in range(TOP):
        picked = lax.dot_general(
            chosen[k].astype(jnp.bfloat16),
            returned,
            (((0,), (0,)), ((), ())),
            preferred_element_type=jnp.float32,
        )
        routed_sum = routed_sum + combine[:, k : k + 1] * picked
    return (total + routed_sum).astype(jnp.bfloat16)


def solution(mesh):
    return jax.shard_map(
        body,
        mesh=mesh,
        in_specs=(
            P("sp", "tp"),
            P("sp", None),
            P("sp", None),
            P(),
            P(None, "tp"),
            P(None, "tp"),
            P("sp", "tp"),
            P(),
            P("sp", None),
            P("sp", None),
            P("sp"),
            P("sp", None, "tp"),
            P("sp", None, "tp"),
            P("sp", None, "tp"),
        ),
        out_specs=P("sp", "tp"),
        check_vma=False,
    )
```
